32 devices in a mesh: grp: 2 (over x), ep: 16 (over z, y, core).
Axes of the slice: x: 2, y: 2, z: 4, core: 2. Of those that a mesh axis runs over, the one named last changes fastest.
Arguments:
- hidden: bfloat16 [224, 2048], P(('grp', 'ep')), parts along dimension 0, may hold values from -6 to 6
- state_in: float32 [224, 64, 4096], P(('grp', 'ep')), parts along dimension 0, may hold values from -4 to 4
- conv_state: bfloat16 [224, 3, 4608], P(('grp', 'ep')), parts along dimension 0, may hold values from -6 to 6
- expert_ids: int32 [224, 4], P(('grp', 'ep')), parts along dimension 0, may hold values from 0 to 15, as said below
- group_prob: float32 [224], P(('grp', 'ep')), parts along dimension 0, may hold values from 0.25 to 1
- expert_score: float32 [224, 4], P(('grp', 'ep')), parts along dimension 0, may hold values from 0.05 to 1
- first_gain: bfloat16 [2048], replicated, may hold values from 0.099609375 to 1.8984375
- z_weight: bfloat16 [2048, 4096], P(None, 'ep'), may hold values from -0.125 to 0.125
- x_weight: bfloat16 [2048, 4096], P(None, 'ep'), may hold values from -0.125 to 0.125
- b_weight: bfloat16 [2048, 256], replicated, may hold values from -0.125 to 0.125
- c_weight: bfloat16 [2048, 256], replicated, may hold values from -0.125 to 0.125
- dt_weight: bfloat16 [2048, 64], replicated, may hold values from -0.125 to 0.125
- conv_weight: bfloat16 [4, 4608], replicated, may hold values from -3 to 3
- conv_bias: bfloat16 [4608], replicated, may hold values from -3 to 3
- dt_bias: float32 [64], replicated, may hold values from -4 to 0
- decay_log: float32 [64], replicated, may hold values from 0 to 2
- skip_gain: float32 [64], replicated, may hold values from 0.1 to 1.9
- inner_gain: bfloat16 [4096], replicated, may hold values from 0.099609375 to 1.8984375
- out_weight: bfloat16 [4096, 2048], P(None, 'ep'), may hold values from -0.09375 to 0.09375
- second_gain: bfloat16 [2048], replicated, may hold values from 0.099609375 to 1.8984375
- expert_gate: bfloat16 [16, 2048, 512], P('ep'), may hold values from -0.125 to 0.125
- expert_up: bfloat16 [16, 2048, 512], P('ep'), may hold values from -0.125 to 0.125
- expert_down: bfloat16 [16, 512, 2048], P('ep'), may hold values from -0.25 to 0.25
Outputs:
- layer_out: bfloat16 [224, 2048], P(('grp', 'ep')), parts along dimension 0
- state_out: float32 [224, 64, 4096], P(('grp', 'ep')), parts along dimension 0
- conv_out: bfloat16 [224, 3, 4608], P(('grp', 'ep')), parts along dimension 0
The draws below stay inside these ranges and needn't reach their ends.
There are 2 independent parts, one for each index of `grp`. The reference program is written for one: setup_inputs(seed, part) draws one part's arguments, and reference() takes and returns one part's arrays. A program takes and returns all parts, laid end to end along the dimension named above; an argument that names none is the same for every part. Nothing has to cross between parts.
Inputs may be any that keep to these rules, and one draw needn't show every extreme that they name: `expert_ids`: each row names 4 different experts of one expert group (numbers g * 8 to g * 8 + 7). Among the 7 rows of one device no expert is named more than 3 times, and in every draw one expert is named exactly 3 times by the rows of every device.
All inputs are finite; a program needn't handle non-finite values.
Results may differ from the reference program's by a relative error of at most 0.014.
Values may be sent and summed in bfloat16 or wider, within the bound.
No kernel may reach another device: no remote copies, remote signals or barrier semaphores. Data moves between devices by JAX's collectives and lax.ppermute only.
A program may use at most 128 MiB of HBM per device.

```python
import math
import jax
import jax.numpy as jnp
from jax import lax

D = 2048
HEADS = 64
HEAD_DIM = 64
SSM_GROUPS = 4
STATE = 64
CONV = 4
MOE_HIDDEN = 512
EXP_GROUP = 8
TOP = 4
SEQ_DEV = 7
INNER = 4096
CONV_DIM = 4608
EXPERTS = 16
TOKENS = 112
CAP = 3
N_EP = 16


def draw_expert_ids(key, part):
    group_count = N_EP // EXP_GROUP
    hot_rows = min(SEQ_DEV, CAP + CAP * (EXP_GROUP - TOP) // TOP)
    hot_key, rest_key = jax.random.split(jax.random.fold_in(key, 11))
    hot_expert = jax.random.randint(hot_key, (), 0, N_EP)
    hot_group = hot_expert // EXP_GROUP
    hot_local = hot_expert % EXP_GROUP
    row_index = jnp.arange(SEQ_DEV, dtype=jnp.int32)[:, None]
    pick_index = jnp.arange(TOP, dtype=jnp.int32)[None, :]

    def one_block(block_key):
        key_order, key_inner, key_hot, key_shuffle, key_within = jax.random.split(block_key, 5)
        group_order = jax.random.permutation(key_order, group_count)
        sort_keys = (group_order == hot_group).astype(jnp.int32) * group_count + jnp.arange(group_count, dtype=jnp.int32)
        other_groups = group_order[jnp.argsort(sort_keys)][:group_count - 1]
        inner_keys = jax.random.split(key_inner, group_count - 1)
        inner_perm = jax.vmap(lambda one_key: jax.random.permutation(one_key, EXP_GROUP))(inner_keys)
        hot_perm = jax.random.permutation(key_hot, EXP_GROUP - 1)
        early_place = jnp.where(pick_index == 0, 0, 1 + (row_index * (TOP - 1) + pick_index - 1) % (EXP_GROUP - 1))
        late_place = 1 + (CAP * (TOP - 1) + (row_index - CAP) * TOP + pick_index) % (EXP_GROUP - 1)
        hot_place = jnp.where(row_index < CAP, early_place, late_place)
        hot_local_pick = jnp.where(hot_place == 0, hot_local, (hot_local + 1 + hot_perm[jnp.maximum(hot_place - 1, 0)]) % EXP_GROUP)
        hot_pick = hot_group * EXP_GROUP + hot_local_pick
        cold_row = jnp.maximum(row_index - hot_rows, 0)
        cold_group = cold_row % (group_count - 1)
        cold_turn = cold_row // (group_count - 1)
        cold_place = (cold_turn * TOP + pick_index) % EXP_GROUP
        cold_pick = other_groups[cold_group] * EXP_GROUP + inner_perm[cold_group, cold_place]
        block_ids = jnp.where(row_index < hot_rows, hot_pick, cold_pick)
        shuffle = jax.random.permutation(key_shuffle, SEQ_DEV)
        block_ids = block_ids[shuffle]
        within_keys = jax.random.split(key_within, SEQ_DEV)
        within = jax.vmap(lambda one_key: jax.random.permutation(one_key, TOP))(within_keys)
        return jnp.take_along_axis(block_ids, within, axis=1)
    block_keys = jax.random.split(rest_key, N_EP)
    return jax.vmap(one_block)(block_keys).reshape(N_EP * SEQ_DEV, TOP).astype(jnp.int32)


def block_levels(key, extent, cuts, least, high):
    level = 1.0
    for dim, blocks in cuts:
        heights = jax.random.uniform(jax.random.fold_in(jax.random.fold_in(key, 6), dim), (blocks,), jnp.float32, least / len(cuts), high / len(cuts))
        level = level * jnp.repeat(jnp.exp(heights), extent[dim] // blocks).reshape((-1,) + (1,) * (len(extent) - 1 - dim))
    return level


def normal_values(own_key, shape, width, limit, pieces=(), kind=jnp.bfloat16):
    loudness = block_levels(own_key, shape, pieces, -0.22, 0.18) if pieces else 1.0
    result = jax.random.normal(own_key, shape, jnp.float32) * width * loudness
    return jnp.minimum(jnp.maximum(result, -limit), limit).astype(kind)


def setup_inputs(seed: int = 0, part: int = 0) -> dict:
    key_list = jax.random.split(jax.random.key(seed), 24)
    part_splits = jax.random.split(jax.random.fold_in(key_list[23], part), 24)
    return {
        "hidden": normal_values(part_splits[0], (TOKENS, D), 1.0, 6.0, ((0, 16),)),
        "state_in": normal_values(part_splits[1], (TOKENS, HEADS, HEAD_DIM * STATE), 0.3, 4.0, ((0, 16),), jnp.float32),
        "conv_state": normal_values(part_splits[2], (TOKENS, CONV - 1, CONV_DIM), 1.0, 6.0, ((0, 16),)),
        "expert_ids": draw_expert_ids(jax.random.fold_in(jax.random.fold_in(key_list[23], part), 71), part),
        "group_prob": jnp.clip(jnp.exp(math.log(1.0) - 1.3862944 * jax.random.uniform(part_splits[4], (TOKENS,), jnp.float32) ** block_levels(part_splits[4], (TOKENS,), ((0, 16),), -0.2, 0.2)), 0.25, 1.0),
        "expert_score": jnp.clip(jnp.exp(math.log(1.0) - 2.9957323 * jax.random.uniform(part_splits[5], (TOKENS, TOP), jnp.float32) ** block_levels(part_splits[5], (TOKENS, TOP), ((0, 16),), -0.2, 0.2)), 0.05, 1.0),
        "first_gain": jnp.clip(1.0 + 0.18 * jax.random.normal(key_list[6], (D,), jnp.float32), 0.099609375, 1.8984375).astype(jnp.bfloat16),
        "z_weight": normal_values(key_list[7], (D, INNER), D ** -0.5, 0.125, ((1, 16),)),
        "x_weight": normal_values(key_list[8], (D, INNER), D ** -0.5, 0.125, ((1, 16),)),
        "b_weight": normal_values(key_list[9], (D, SSM_GROUPS * STATE), D ** -0.5, 0.125),
        "c_weight": normal_values(key_list[10], (D, SSM_GROUPS * STATE), D ** -0.5, 0.125),
        "dt_weight": normal_values(key_list[11], (D, HEADS), D ** -0.5, 0.125),
        "conv_weight": normal_values(key_list[12], (CONV, CONV_DIM), 0.5, 3.0),
        "conv_bias": normal_values(key_list[13], (CONV_DIM,), 0.5, 3.0),
        "dt_bias": jnp.clip(jax.random.uniform(key_list[14], (HEADS,), jnp.float32, -4.0, 0.0), -4.0, 0.0),
        "decay_log": jnp.clip(jax.random.uniform(key_list[15], (HEADS,), jnp.float32, 0.0, 2.0), 0.0, 2.0),
        "skip_gain": jnp.clip(1.0 + 0.18 * jax.random.normal(key_list[16], (HEADS,), jnp.float32), 0.1, 1.9),
        "inner_gain": jnp.clip(1.0 + 0.18 * jax.random.normal(key_list[17], (INNER,), jnp.float32), 0.099609375, 1.8984375).astype(jnp.bfloat16),
        "out_weight": normal_values(key_list[18], (INNER, D), INNER ** -0.5, 0.09375, ((1, 16),)),
        "second_gain": jnp.clip(1.0 + 0.18 * jax.random.normal(key_list[19], (D,), jnp.float32), 0.099609375, 1.8984375).astype(jnp.bfloat16),
        "expert_gate": normal_values(key_list[20], (EXPERTS, D, MOE_HIDDEN), D ** -0.5, 0.125, ((0, 16),)),
        "expert_up": normal_values(key_list[21], (EXPERTS, D, MOE_HIDDEN), D ** -0.5, 0.125, ((0, 16),)),
        "expert_down": normal_values(key_list[22], (EXPERTS, MOE_HIDDEN, D), MOE_HIDDEN ** -0.5, 0.25, ((0, 16),)),
    }


EPS = 1e-06

def rms_scale(values, gain_vec):
    return values * lax.rsqrt(lax.optimization_barrier(jnp.mean(values * values, axis=-1, keepdims=True)) + EPS) * gain_vec.astype(jnp.float32)

def state_step(active, dt_raw, state_in, dt_bias, decay_log, skip_gain):
    row_count = active.shape[0]
    inner_width = HEADS * HEAD_DIM
    state_span = SSM_GROUPS * STATE
    per_group = HEADS // SSM_GROUPS
    x_heads = active[:, :inner_width].reshape(row_count, HEADS, HEAD_DIM)
    b_input = active[:, inner_width:inner_width + state_span].reshape(row_count, SSM_GROUPS, STATE)
    c_input = active[:, inner_width + state_span:].reshape(row_count, SSM_GROUPS, STATE)
    b_heads = jnp.repeat(b_input, per_group, axis=1)
    c_heads = jnp.repeat(c_input, per_group, axis=1)
    step_size = jax.nn.softplus(dt_raw.astype(jnp.float32) + dt_bias[None, :])
    decay_rate = jnp.exp(-step_size * jnp.exp(decay_log)[None, :])
    carried = state_in.reshape(row_count, HEADS, HEAD_DIM, STATE)
    carried = decay_rate[:, :, None, None] * carried + (step_size[:, :, None] * x_heads)[:, :, :, None] * b_heads[:, :, None, :]
    readout = jnp.einsum('bhpn,bhn->bhp', carried, c_heads, precision=lax.Precision.HIGHEST)
    readout = readout + skip_gain[None, :, None] * x_heads
    return (readout.reshape(row_count, inner_width), carried.reshape(row_count, HEADS, HEAD_DIM * STATE))

def reference(hidden, state_in, conv_state, expert_ids, group_prob, expert_score, first_gain, z_weight, x_weight, b_weight, c_weight, dt_weight, conv_weight, conv_bias, dt_bias, decay_log, skip_gain, inner_gain, out_weight, second_gain, expert_gate, expert_up, expert_down):
    row_count = hidden.shape[0]
    normed = rms_scale(hidden.astype(jnp.float32), first_gain).astype(jnp.bfloat16)
    gate_z = jnp.dot(normed, z_weight, preferred_element_type=jnp.float32).astype(jnp.bfloat16)
    x_part = jnp.dot(normed, x_weight, preferred_element_type=jnp.float32).astype(jnp.bfloat16)
    b_part = jnp.dot(normed, b_weight, preferred_element_type=jnp.float32).astype(jnp.bfloat16)
    c_part = jnp.dot(normed, c_weight, preferred_element_type=jnp.float32).astype(jnp.bfloat16)
    dt_raw = jnp.dot(normed, dt_weight, preferred_element_type=jnp.float32).astype(jnp.bfloat16)
    fresh_input = jnp.concatenate([x_part, b_part, c_part], axis=1)
    window = jnp.concatenate([conv_state, fresh_input[:, None, :]], axis=1)
    summed = lax.optimization_barrier(jnp.sum(window.astype(jnp.float32) * conv_weight.astype(jnp.float32)[None], axis=1))
    active = jax.nn.silu(summed + conv_bias.astype(jnp.float32)[None, :])
    readout, state_out = state_step(active, dt_raw, state_in, dt_bias, decay_log, skip_gain)
    gated = readout * jax.nn.silu(gate_z.astype(jnp.float32))
    y_mix = rms_scale(gated, inner_gain).astype(jnp.bfloat16)
    projected = jnp.dot(y_mix, out_weight, preferred_element_type=jnp.float32).astype(jnp.bfloat16)
    projected = lax.optimization_barrier(projected)
    mixed_rows = (hidden.astype(jnp.float32) + projected.astype(jnp.float32)).astype(jnp.bfloat16)
    normed2 = rms_scale(mixed_rows.astype(jnp.float32), second_gain).astype(jnp.bfloat16)
    route_share = group_prob[:, None] * expert_score / lax.optimization_barrier(jnp.sum(expert_score, axis=1, keepdims=True))
    flat_ids = expert_ids.reshape(-1).astype(jnp.int32)
    flat_share = route_share.reshape(-1)
    route_count = flat_ids.shape[0]
    flat_rows = jnp.repeat(jnp.arange(row_count, dtype=jnp.int32), TOP)
    max_rows = N_EP * CAP

    def per_expert(accum, expert):
        is_routed = (flat_ids == expert).astype(jnp.int32)
        sort_keys = (1 - is_routed) * route_count + jnp.arange(route_count, dtype=jnp.int32)
        chosen = jnp.argsort(sort_keys)[:max_rows].astype(jnp.int32)
        token_rows = flat_rows[chosen]
        picked = normed2[token_rows]
        gate_part = jnp.dot(picked, expert_gate[expert], preferred_element_type=jnp.float32)
        up_part = jnp.dot(picked, expert_up[expert], preferred_element_type=jnp.float32)
        hidden_act = (jax.nn.silu(gate_part) * up_part).astype(jnp.bfloat16)
        expert_out = jnp.dot(hidden_act, expert_down[expert], preferred_element_type=jnp.float32).astype(jnp.bfloat16)
        expert_out = lax.optimization_barrier(expert_out)
        weight_vec = flat_share[chosen] * is_routed[chosen].astype(jnp.float32)
        accum = accum.at[token_rows].add(weight_vec[:, None] * expert_out.astype(jnp.float32))
        return (accum, None)
    blank = jnp.zeros((row_count, hidden.shape[1]), jnp.float32)
    moe_sum, _ = lax.scan(per_expert, blank, jnp.arange(EXPERTS, dtype=jnp.int32))
    layer_out = (mixed_rows.astype(jnp.float32) + moe_sum).astype(jnp.bfloat16)
    return (layer_out, state_out, window[:, 1:, :])
```

```python
import functools

import jax
import jax.numpy as jnp
from jax import lax
from jax.experimental import pallas as pl
from jax.experimental.pallas import tpu as pltpu
from jax.sharding import PartitionSpec as P


HEADS = 64
HEAD_DIM = 64
SSM_GROUPS = 4
STATE = 64
TOP = 4
EPS = 1e-06
PAD = 8
LANES = 128
F32 = jnp.float32
BF16 = jnp.bfloat16


def silu(v):
    return v * jax.nn.sigmoid(v)


def call(kernel, out_shape, limit_mib, flops, moved, **kw):
    return pl.pallas_call(
        kernel,
        out_shape=out_shape,
        compiler_params=pltpu.CompilerParams(vmem_limit_bytes=limit_mib * 2**20),
        cost_estimate=pl.CostEstimate(flops=flops, bytes_accessed=moved, transcendentals=0),
        **kw,
    )


def vmem():
    return pl.BlockSpec(memory_space=pltpu.VMEM)


def swap(values, bits, count):
    return lax.ppermute(values, "ep", [(i, i ^ bits) for i in range(count)])


def join_kernel(*refs):
    for k, ref in enumerate(refs[:-1]):
        refs[-1][k] = ref[...]


def join(blocks, shape):
    return call(
        join_kernel,
        jax.ShapeDtypeStruct((len(blocks),) + shape, blocks[0].dtype),
        4,
        blocks[0].size,
        blocks[0].size,
        in_specs=[vmem()] * len(blocks),
        out_specs=vmem(),
        name="join",
    )(*blocks)


def gather(block, count, ahead, local_copy=None):
    blocks = [block if local_copy is None else local_copy]
    for k in reversed(range(1, count // 4)):
        blocks.append(swap(block, 4 * k, count))
    side = []
    for k in range(ahead):
        side.append(swap(blocks[k], 2, count))
    rest = early = join(blocks[ahead:], block.shape)
    rest = swap(rest, 2, count)
    if ahead:
        early = join(blocks + side, block.shape)
    early_core = swap(early, 1, count)
    return early, rest, early_core, swap(rest, 1, count)


def owners(me, parts, count, ahead):
    near = [0] + [4 * k for k in reversed(range(1, count // 4))]
    early = near + [bits ^ 2 for bits in near[:ahead]]
    rest = [bits ^ 2 for bits in near[ahead:]]
    every = early, rest, [bits ^ 1 for bits in early], [bits ^ 1 for bits in rest]
    for bits, part in zip(every, parts):
        for k in range(part.shape[0]):
            yield part, k, me ^ bits[k]


AHEAD = {"first": 0, "second": 2}


def widen_rows(ref, rows):
    groups, _, lanes = ref.shape
    per_group = HEADS // groups
    lines = [
        jnp.broadcast_to(ref[g, t : t + 1, :], (per_group, lanes))
        for t in range(rows)
        for g in range(groups)
    ]
    return jnp.concatenate(lines, axis=0).reshape(rows, HEADS, lanes)


def three_parts(values):
    high = values.astype(BF16)
    rest = values - high.astype(F32)
    mid = rest.astype(BF16)
    low = (rest - mid.astype(F32)).astype(BF16)
    return high, mid, low


def one_row(ref):
    values = ref[...].astype(F32)
    return jnp.concatenate([values[k : k + 1] for k in range(values.shape[0])], axis=1)


def to_column(row, rows):
    size = row.shape[1]
    i = lax.broadcasted_iota(jnp.int32, (rows, size), 0)
    j = lax.broadcasted_iota(jnp.int32, (rows, size), 1)
    return jnp.sum(jnp.where(i == j, jnp.broadcast_to(row, (rows, size)), 0.0), axis=1, keepdims=True)


def local_kernel(
    hidden_ref, gain_ref, b_ref, c_ref, dt_ref, conv_ref, taps_ref, bias_ref, dt_bias_ref,
    log_ref, skip_ref, ids_ref, prob_ref, score_ref,
    early_ref, coef_ref, step_ref, b_wide_ref, c_wide_ref, decay_ref, bc_ref, ids_out_ref, share_ref,
    own_ref,
):
    rows, _ = hidden_ref.shape
    inner = HEADS * HEAD_DIM
    span = SSM_GROUPS * STATE
    per_group = HEADS // SSM_GROUPS
    own_ref[...] = hidden_ref[...]
    values = hidden_ref[...].astype(F32)
    scale = lax.rsqrt(jnp.mean(values * values, axis=-1, keepdims=True) + EPS)
    normed = (values * scale * one_row(gain_ref)).astype(BF16)
    b_part = jnp.dot(normed, b_ref[...], preferred_element_type=F32).astype(BF16)
    c_part = jnp.dot(normed, c_ref[...], preferred_element_type=F32).astype(BF16)
    dt_raw = lax.dot_general(
        normed, dt_ref[...], (((1,), (1,)), ((), ())), preferred_element_type=F32
    ).astype(BF16)
    bc_ref[:, :span] = b_part
    bc_ref[:, span:] = c_part
    taps = taps_ref[...].astype(F32)
    last = taps.shape[0] - 1
    early = one_row(bias_ref)
    for k in range(last):
        early = early + conv_ref[k].astype(F32) * taps[k : k + 1]
    early_ref[...] = jnp.zeros_like(early_ref)
    early_ref[:rows] = early[:, :inner]
    fresh = jnp.concatenate([b_part, c_part], axis=1).astype(F32)
    active = silu(early[:, inner:] + fresh * taps[last:, inner:])
    b_act = active[:, :span]
    c_act = active[:, span:]
    step = jax.nn.softplus(dt_raw.astype(F32) + dt_bias_ref[...])
    decay = jnp.exp(-step * jnp.exp(log_ref[...]))
    coefs = []
    for g in range(SSM_GROUPS):
        cut = slice(g * STATE, (g + 1) * STATE)
        b_wide_ref[g] = jnp.concatenate([b_act[:, cut]] * (LANES // STATE), axis=1)
        c_wide_ref[g] = jnp.concatenate([c_act[:, cut]] * (LANES // STATE), axis=1)
        dots = jnp.sum(b_act[:, cut] * c_act[:, cut], axis=1, keepdims=True)
        coefs.append(jnp.broadcast_to(dots, (rows, per_group)))
    coef = step * jnp.concatenate(coefs, axis=1) + skip_ref[...]
    chan = lax.broadcasted_iota(jnp.int32, (3 * HEADS, inner), 0)
    lane = lax.broadcasted_iota(jnp.int32, (3 * HEADS, inner), 1)
    spread = (lane // HEAD_DIM == chan % HEADS).astype(F32).astype(BF16)
    for values, ref in ((coef, coef_ref), (step, step_ref)):
        parts = jnp.concatenate(three_parts(values), axis=1)
        ref[...] = jnp.zeros_like(ref)
        ref[:rows] = jnp.dot(parts, spread, preferred_element_type=F32)
    for t in range(rows):
        decay_ref[t] = jnp.broadcast_to(to_column(decay[t : t + 1], HEADS), (HEADS, LANES))
    width = share_ref.shape[1]
    split = share_ref.shape[0] // (3 * PAD)
    at = lax.broadcasted_iota(jnp.int32, (rows, width), 1)
    expert = (at // PAD).astype(F32)
    ids = [to_column(ids_ref[k : k + 1].astype(F32), rows) for k in range(TOP)]
    scores = score_ref[...]
    shares = prob_ref[...] * scores / jnp.sum(scores, axis=0, keepdims=True)
    shares = [to_column(shares[k : k + 1], rows) for k in range(TOP)]
    weight = jnp.zeros((rows, width), F32)
    used = jnp.zeros((rows, width), F32)
    numbers = jnp.zeros((rows, LANES), F32)
    lane = lax.broadcasted_iota(jnp.int32, (rows, LANES), 1)
    line = lax.broadcasted_iota(jnp.int32, (rows, LANES), 0)
    for k in range(TOP):
        hit = jnp.broadcast_to(ids[k], (rows, width)) == expert
        weight += jnp.where(hit, jnp.broadcast_to(shares[k], (rows, width)), 0.0)
        used += jnp.where(hit, 1.0, 0.0)
        numbers += jnp.where(lane == k * PAD + line, jnp.broadcast_to(ids[k] + 1.0, (rows, LANES)), 0.0)
    ids_out_ref[...] = jnp.sum(numbers, axis=0, keepdims=True) - 1.0
    seen = jnp.zeros((1, width), F32)
    ranks = []
    for t in range(rows):
        ranks.append(seen)
        seen = seen + used[t : t + 1]
    rank = jnp.concatenate(ranks, axis=0)
    weight = jnp.where(rank == (at % PAD // split).astype(F32), weight, 0.0)
    share_ref[...] = jnp.zeros_like(share_ref)
    for s in range(split):
        cut = jnp.where(at % split == s, weight, 0.0)
        for i, part in enumerate(three_parts(cut)):
            share_ref[(3 * s + i) * PAD : (3 * s + i) * PAD + rows] = part


def read_kernel(
    state_ref, c_ref, decay_ref, keep_ref, out_ref, c_wide_ref, sums_ref, flat_ref, sems
):
    rows, heads, width = state_ref.shape
    lanes = 512

    def copy(chunk):
        cut = pl.ds(pl.multiple_of(chunk * lanes, lanes), lanes)
        return pltpu.make_async_copy(
            state_ref.at[:, :, cut], keep_ref.at[:, :, cut], sems.at[chunk]
        )

    def begin(chunk, carry):
        copy(chunk).start()
        return carry

    lax.fori_loop(0, width // lanes, begin, 0)
    c_wide_ref[...] = widen_rows(c_ref, rows)
    sums_ref[...] = jnp.zeros_like(sums_ref)

    def one(chunk, carry):
        copy(chunk).wait()
        at = pl.multiple_of(chunk * lanes, lanes)
        prods = []
        for k in range(lanes // LANES):
            prod = keep_ref[:, :, pl.ds(at + k * LANES, LANES)] * c_wide_ref[...]
            prods.append(prod.reshape(rows * heads, LANES).astype(BF16))
        lane = lax.broadcasted_iota(jnp.int32, (lanes, HEAD_DIM), 0)
        chan = lax.broadcasted_iota(jnp.int32, (lanes, HEAD_DIM), 1)
        pick = (chunk * (lanes // STATE) + lane // STATE == chan).astype(F32).astype(BF16)
        prods = jnp.concatenate(prods, axis=1)
        sums_ref[...] += jnp.dot(prods, pick, preferred_element_type=F32)
        return carry

    lax.fori_loop(0, width // lanes, one, 0)
    flat_ref[...] = sums_ref[...] * decay_ref[...].reshape(rows * heads, LANES)[:, :HEAD_DIM]
    out_ref[...] = jnp.zeros_like(out_ref)
    for h in range(0, heads, 2):
        pair = [flat_ref[pl.ds(h + j, rows, stride=heads), :] for j in range(2)]
        out_ref[:rows, h * HEAD_DIM : (h + 2) * HEAD_DIM] = jnp.concatenate(pair, axis=1)


def read_state(state_in, c_wide, decay_wide):
    rows, heads, width = state_in.shape
    return call(
        read_kernel,
        (
            jax.ShapeDtypeStruct(state_in.shape, F32),
            jax.ShapeDtypeStruct((PAD, heads * HEAD_DIM), F32),
        ),
        12,
        20_000_000,
        state_in.size * 4,
        in_specs=[pl.BlockSpec(memory_space=pltpu.HBM), vmem(), vmem()],
        out_specs=(vmem(), vmem()),
        scratch_shapes=[
            pltpu.VMEM((rows, heads, LANES), F32),
            pltpu.VMEM((rows * heads, HEAD_DIM), F32),
            pltpu.VMEM((rows * heads, HEAD_DIM), F32),
            pltpu.SemaphoreType.DMA((width // 512,)),
        ],
        name="read_state",
    )(state_in, c_wide, decay_wide)


def write_kernel(
    state_ref, xs_ref, b_ref, decay_ref, conv_ref, fresh_ref, bc_ref,
    out_ref, conv_out_ref, parts_ref, b_wide_ref, new_ref, sems,
):
    rows, heads, width = state_ref.shape
    lanes = 512
    inner = heads * HEAD_DIM
    for h in range(heads):
        parts_ref[pl.ds(h, rows, stride=heads), :] = xs_ref[
            :rows, h * HEAD_DIM : (h + 1) * HEAD_DIM
        ]
    parts = jnp.concatenate(three_parts(parts_ref[...]), axis=1)
    b_wide_ref[...] = widen_rows(b_ref, rows)

    def copy(chunk):
        cut = pl.ds(pl.multiple_of(chunk * lanes, lanes), lanes)
        return pltpu.make_async_copy(
            new_ref.at[:, :, cut], out_ref.at[:, :, cut], sems.at[chunk]
        )

    def one(chunk, carry):
        at = pl.multiple_of(chunk * lanes, lanes)
        lane = lax.broadcasted_iota(jnp.int32, (3 * HEAD_DIM, lanes), 1)
        chan = lax.broadcasted_iota(jnp.int32, (3 * HEAD_DIM, lanes), 0)
        spread = chunk * (lanes // STATE) + lane // STATE == chan % HEAD_DIM
        wide = jnp.dot(parts, spread.astype(F32).astype(BF16), preferred_element_type=F32)
        wide = wide.reshape(rows, heads, lanes)
        for k in range(lanes // LANES):
            cut = pl.ds(at + k * LANES, LANES)
            new_ref[:, :, cut] = (
                decay_ref[...] * state_ref[:, :, cut]
                + wide[:, :, k * LANES : (k + 1) * LANES] * b_wide_ref[...]
            )
        copy(chunk).start()
        return carry

    lax.fori_loop(0, width // lanes, one, 0)
    taps = conv_ref.shape[0]
    for k in range(1, taps):
        conv_out_ref[k - 1] = conv_ref[k]
    conv_out_ref[taps - 1, :, :inner] = fresh_ref[:rows]
    conv_out_ref[taps - 1, :, inner:] = bc_ref[...]

    def done(chunk, carry):
        copy(chunk).wait()
        return carry

    lax.fori_loop(0, width // lanes, done, 0)


def write_state(state, xs, b_wide, decay_wide, conv, fresh, bc):
    rows, heads, width = state.shape
    return call(
        write_kernel,
        (jax.ShapeDtypeStruct(state.shape, F32), jax.ShapeDtypeStruct(conv.shape, BF16)),
        16,
        40_000_000,
        state.size * 4,
        in_specs=[vmem()] * 7,
        out_specs=(pl.BlockSpec(memory_space=pltpu.HBM), vmem()),
        scratch_shapes=[
            pltpu.VMEM((rows * heads, HEAD_DIM), F32),
            pltpu.VMEM((rows, heads, LANES), F32),
            pltpu.VMEM(state.shape, F32),
            pltpu.SemaphoreType.DMA((width // 512,)),
        ],
        name="write_state",
    )(state, xs, b_wide, decay_wide, conv, fresh, bc)


def project_kernel(*refs):
    *parts, z_ref, x_ref, gain_ref, ids_ref, out_ref, rows_ref = refs
    me = lax.axis_index("ep")
    count = rows_ref.shape[0]
    rows, model_width = parts[0].shape[1:]
    cols = z_ref.shape[1]
    rows_ref[:, rows:, :] = jnp.zeros((count, PAD - rows, model_width), BF16)
    for part, k, owner in owners(me, parts, count, AHEAD["first"]):
        rows_ref[owner, :rows] = part[k]
    values = rows_ref[...].astype(F32).reshape(count * PAD, model_width)
    scale = lax.rsqrt(jnp.mean(values * values, axis=-1, keepdims=True) + EPS)
    normed = (values * scale * one_row(gain_ref)).astype(BF16)
    z_cols = jnp.dot(normed, z_ref[...], preferred_element_type=F32)
    x_cols = jnp.dot(normed, x_ref[...], preferred_element_type=F32).astype(BF16)
    spare = lax.broadcasted_iota(jnp.int32, (count * PAD, LANES), 0) % PAD == rows
    ids = jnp.broadcast_to(ids_ref[...], (count * PAD, LANES))
    first = jnp.where(spare, ids, z_cols[:, :LANES])
    z_cols = jnp.concatenate([first, z_cols[:, LANES:]], axis=1) if cols > LANES else first
    out_ref[:, :, :cols] = z_cols.astype(BF16).reshape(count, PAD, cols)
    out_ref[:, :, cols:] = x_cols.reshape(count, PAD, cols)


def gate_kernel(
    zx_ref, early_ref, taps_ref, coef_ref, read_ref, step_ref, gain_ref, y_ref, xs_ref, fresh_ref
):
    count, _, both = zx_ref.shape
    cols = both // 2
    inner = count * cols
    z = jnp.concatenate([zx_ref[j, :, :cols] for j in range(count)], axis=1)
    x = jnp.concatenate([zx_ref[j, :, cols:] for j in range(count)], axis=1)
    fresh_ref[...] = x
    last = taps_ref.shape[0] - 1
    tap = taps_ref[...].astype(F32)[last:, :inner]
    x_act = silu(early_ref[...] + x.astype(F32) * tap)
    xs_ref[...] = step_ref[...] * x_act
    gated = (read_ref[...] + coef_ref[...] * x_act) * silu(z.astype(F32))
    scale = lax.rsqrt(jnp.mean(gated * gated, axis=-1, keepdims=True) + EPS)
    y_ref[...] = (gated * scale * one_row(gain_ref)).astype(BF16)


def output_kernel(*refs):
    *parts, weight_ref, pick_ref, out_ref, cols_ref = refs
    count, slots, col = out_ref.shape
    width = weight_ref.shape[0]
    rows = jnp.concatenate(
        [part[...].reshape(part.shape[0] * PAD, width) for part in parts], axis=0
    )
    cols = jnp.dot(rows, weight_ref[...], preferred_element_type=F32)
    blocks = owners(lax.axis_index("ep"), parts, count, AHEAD["second"])
    for i, (_, _, owner) in enumerate(blocks):
        cols_ref[owner] = cols[i * PAD : (i + 1) * PAD]
    cols = cols_ref[...].reshape(count * PAD, col).astype(BF16)
    pick = pick_ref[...].reshape(count * slots, count * PAD)
    picked = jnp.dot(pick, cols, preferred_element_type=F32)
    out_ref[...] = picked.astype(BF16).reshape(count, slots, col)


def choose_kernel(zx_ref, rows_ref, pick_ref, hidden_ref, capacity, rows):
    count, slots, tokens = pick_ref.shape
    ids = jnp.concatenate(
        [zx_ref[j, :, :LANES].astype(F32)[rows : rows + 1] for j in range(count)], axis=0
    ).astype(BF16)
    source = lax.broadcasted_iota(jnp.int32, (LANES, tokens), 0)
    lane = lax.broadcasted_iota(jnp.int32, (LANES, tokens), 1)
    mine = lax.broadcasted_iota(jnp.int32, (count, tokens), 0)
    token = lax.broadcasted_iota(jnp.int32, (count, tokens), 1)
    named = jnp.zeros((count, tokens), F32)
    for k in range(TOP):
        take = (source == k * PAD + lane % PAD).astype(F32).astype(BF16)
        wide = jnp.dot(ids, take, preferred_element_type=F32)
        line = jnp.sum(jnp.where(mine == token // PAD, wide, 0.0), axis=0, keepdims=True)
        named += (jnp.broadcast_to(line, (count, tokens)) == mine.astype(F32)).astype(F32)
    row = lax.broadcasted_iota(jnp.int32, (tokens, tokens), 0)
    col = lax.broadcasted_iota(jnp.int32, (tokens, tokens), 1)
    before = ((row // PAD == col // PAD) & (row < col)).astype(F32).astype(BF16)
    place = jnp.dot(named.astype(BF16), before, preferred_element_type=F32)
    place = jnp.where(named > 0.5, place, -1.0)
    slot = lax.broadcasted_iota(jnp.int32, (slots, tokens), 0)
    lane = lax.broadcasted_iota(jnp.int32, (slots, tokens), 1)
    taken = slots - PAD
    from_sender = (slot // capacity == lane // PAD) & (slot < taken)
    wanted = jnp.where(from_sender, (slot % capacity).astype(F32), -2.0)
    for j in range(count):
        hit = wanted == jnp.broadcast_to(place[j : j + 1], (slots, tokens))
        own = lane - j * PAD == slot - taken
        pick_ref[j] = ((hit | (own & (slot >= taken)))).astype(F32).astype(BF16)
    mine = pick_ref[lax.axis_index("ep")]
    hidden = rows_ref[...].reshape(tokens, rows_ref.shape[2])
    hidden_ref[...] = jnp.dot(mine, hidden, preferred_element_type=F32).astype(BF16)


def expert_kernel(
    hidden_ref, cols_ref, gain_ref, gate_ref, up_ref, down_ref, out_ref, mixed_ref, capacity
):
    count, slots, _ = cols_ref.shape
    model_width = hidden_ref.shape[1]
    projected = jnp.concatenate([cols_ref[j] for j in range(count)], axis=1)
    mixed = (hidden_ref[...].astype(F32) + projected.astype(F32)).astype(BF16)
    mixed_ref[...] = mixed[slots - PAD :]
    wide = mixed.astype(F32)
    scale = lax.rsqrt(jnp.mean(wide * wide, axis=-1, keepdims=True) + EPS)
    normed = (wide * scale * one_row(gain_ref)).astype(BF16)
    gate = jnp.dot(normed, gate_ref[0], preferred_element_type=F32)
    up = jnp.dot(normed, up_ref[0], preferred_element_type=F32)
    act = (silu(gate) * up).astype(BF16)
    width = out_ref.shape[2]
    split = model_width // width
    tokens = count * PAD
    row = lax.broadcasted_iota(jnp.int32, (tokens, slots), 0)
    slot = lax.broadcasted_iota(jnp.int32, (tokens, slots), 1)
    place = row % PAD // split
    spread = (slot == row // PAD * capacity + place) & (place < capacity)
    act = jnp.dot(spread.astype(F32).astype(BF16), act, preferred_element_type=F32).astype(BF16)
    result = jnp.dot(act, down_ref[0], preferred_element_type=F32)
    row = lax.broadcasted_iota(jnp.int32, (tokens, width), 0) % split
    folded = result[:, :width]
    for s in range(1, split):
        folded = jnp.where(row == s, result[:, s * width : (s + 1) * width], folded)
    out_ref[...] = folded.astype(BF16).reshape(count, PAD, width)


def combine_kernel(back_ref, share_ref, mixed_ref, out_ref):
    count, _, width = back_ref.shape
    rows, model_width = out_ref.shape
    values = back_ref[...].reshape(count * PAD, width)
    sums = jnp.dot(share_ref[...], values, preferred_element_type=F32)
    for s in range(model_width // width):
        at = 3 * PAD * s
        total = sums[at : at + PAD] + sums[at + PAD : at + 2 * PAD] + sums[at + 2 * PAD : at + 3 * PAD]
        cut = slice(s * width, (s + 1) * width)
        out_ref[:, cut] = (mixed_ref[:, cut].astype(F32) + total)[:rows].astype(BF16)


def body(
    hidden,
    state_in,
    conv_state,
    expert_ids,
    group_prob,
    expert_score,
    first_gain,
    z_weight,
    x_weight,
    b_weight,
    c_weight,
    dt_weight,
    conv_weight,
    conv_bias,
    dt_bias,
    decay_log,
    skip_gain,
    inner_gain,
    out_weight,
    second_gain,
    expert_gate,
    expert_up,
    expert_down,
):
    rows, model_width = hidden.shape
    inner = HEADS * HEAD_DIM
    span = SSM_GROUPS * STATE
    count = lax.axis_size("ep")
    tokens = count * PAD
    capacity = max(2, (3 * rows * TOP + 2 * count - 1) // (2 * count))
    slots = 2
    while slots < capacity:
        slots *= 2
    split = PAD // slots

    def streamed(array):
        return pltpu.with_memory_space_constraint(array, pltpu.HBM)

    conv_state = conv_state.transpose(1, 0, 2)

    def lines(vector):
        return vector.reshape(-1, LANES)


    def wide(kind):
        return jax.ShapeDtypeStruct((PAD, inner), kind)

    early, coef, step, b_wide, c_wide, decay_wide, bc, ids_row, share_rows, own = call(
        local_kernel,
        (
            wide(F32),
            wide(F32),
            wide(F32),
            jax.ShapeDtypeStruct((SSM_GROUPS, rows, LANES), F32),
            jax.ShapeDtypeStruct((SSM_GROUPS, rows, LANES), F32),
            jax.ShapeDtypeStruct((rows, HEADS, LANES), F32),
            jax.ShapeDtypeStruct((rows, 2 * span), BF16),
            jax.ShapeDtypeStruct((1, LANES), F32),
            jax.ShapeDtypeStruct((split * 3 * PAD, tokens), BF16),
            jax.ShapeDtypeStruct(hidden.shape, BF16),
        ),
        16,
        10_000_000,
        4_000_000,
        in_specs=[vmem()] * 14,
        out_specs=(vmem(),) * 10,
        name="local",
    )(
        *[
            streamed(array)
            for array in (
                hidden,
                lines(first_gain),
                b_weight,
                c_weight,
                dt_weight.T,
                conv_state,
                conv_weight,
                lines(conv_bias),
                dt_bias[None, :],
                decay_log[None, :],
                skip_gain[None, :],
                expert_ids.T,
                group_prob[None, :],
                expert_score.T,
            )
        ]
    )
    parts = gather(hidden, count, AHEAD["first"], own)
    state, read = read_state(streamed(state_in), c_wide, decay_wide)

    cols = z_weight.shape[1]
    zx, all_rows = call(
        project_kernel,
        (
            jax.ShapeDtypeStruct((count, PAD, 2 * cols), BF16),
            jax.ShapeDtypeStruct((count, PAD, model_width), BF16),
        ),
        12,
        4 * tokens * model_width * cols,
        4 * model_width * cols,
        in_specs=[vmem()] * 8,
        out_specs=(vmem(), vmem()),
        name="project",
    )(*parts, z_weight, x_weight, lines(first_gain), ids_row)
    zx = lax.all_to_all(zx, "ep", split_axis=0, concat_axis=0, tiled=True)
    y_mix, xs, x_fresh = call(
        gate_kernel,
        (wide(BF16), wide(F32), wide(BF16)),
        8,
        40 * PAD * inner,
        30 * PAD * inner,
        in_specs=[vmem()] * 7,
        out_specs=(vmem(),) * 3,
        name="gate",
    )(zx, early, conv_weight, coef, read, step, lines(inner_gain))

    taken = count * capacity + PAD
    pick, chosen = call(
        functools.partial(choose_kernel, capacity=capacity, rows=rows),
        (
            jax.ShapeDtypeStruct((count, taken, tokens), BF16),
            jax.ShapeDtypeStruct((taken, model_width), BF16),
        ),
        8,
        2 * taken * tokens * model_width,
        2 * tokens * model_width,
        in_specs=[vmem()] * 2,
        out_specs=(vmem(), vmem()),
        name="choose",
    )(zx, all_rows)

    parts = gather(y_mix, count, AHEAD["second"])
    state_out, conv_out = write_state(
        state, xs, b_wide, decay_wide, conv_state, x_fresh, bc
    )
    out_cols = out_weight.shape[1]
    slab = call(
        output_kernel,
        jax.ShapeDtypeStruct((count, taken, out_cols), BF16),
        12,
        2 * tokens * inner * out_cols,
        2 * inner * out_cols,
        in_specs=[vmem()] * 6,
        out_specs=vmem(),
        scratch_shapes=[pltpu.VMEM((count, PAD, out_cols), F32)],
        name="output",
    )(*parts, out_weight, pick)

    slab = lax.all_to_all(slab, "ep", split_axis=0, concat_axis=0, tiled=True)
    back, mixed = call(
        functools.partial(expert_kernel, capacity=capacity),
        (
            jax.ShapeDtypeStruct((count, PAD, model_width // split), BF16),
            jax.ShapeDtypeStruct((PAD, model_width), BF16),
        ),
        24,
        6 * tokens * expert_gate.shape[1] * expert_gate.shape[2],
        6 * expert_gate.shape[1] * expert_gate.shape[2],
        in_specs=[vmem()] * 6,
        out_specs=(vmem(), vmem()),
        name="expert",
    )(chosen, slab, lines(second_gain), expert_gate, expert_up, expert_down)

    back = lax.all_to_all(back, "ep", split_axis=0, concat_axis=0, tiled=True)
    layer_out = call(
        combine_kernel,
        jax.ShapeDtypeStruct((rows, model_width), BF16),
        8,
        2 * 6 * PAD * tokens * model_width,
        2 * tokens * model_width,
        in_specs=[vmem()] * 3,
        out_specs=vmem(),
        name="combine",
    )(back, share_rows, mixed)
    return layer_out, state_out, conv_out.transpose(1, 0, 2)


def solution(mesh):
    seq = ("grp", "ep")
    in_specs = (
        P(seq, None),
        P(seq, None, None),
        P(seq, None, None),
        P(seq, None),
        P(seq),
        P(seq, None),
        P(),
        P(None, "ep"),
        P(None, "ep"),
        P(),
        P(),
        P(),
        P(),
        P(),
        P(),
        P(),
        P(),
        P(),
        P(None, "ep"),
        P(),
        P("ep", None, None),
        P("ep", None, None),
        P("ep", None, None),
    )
    out_specs = (P(seq, None), P(seq, None, None), P(seq, None, None))

    return jax.shard_map(body, mesh=mesh, in_specs=in_specs, out_specs=out_specs, check_vma=False)
```

```python
import functools

import jax
import jax.numpy as jnp
from jax import lax
from jax.experimental import pallas as pl
from jax.experimental.pallas import tpu as pltpu
from jax.sharding import PartitionSpec as P


HEADS = 64
HEAD_DIM = 64
SSM_GROUPS = 4
STATE = 64
TOP = 4
EPS = 1e-06
PAD = 8
LANES = 128
F32 = jnp.float32
BF16 = jnp.bfloat16


def silu(v):
    return v * jax.nn.sigmoid(v)


def call(kernel, out_shape, limit_mib, flops, moved, **kw):
    return pl.pallas_call(
        kernel,
        out_shape=out_shape,
        compiler_params=pltpu.CompilerParams(vmem_limit_bytes=limit_mib * 2**20),
        cost_estimate=pl.CostEstimate(flops=flops, bytes_accessed=moved, transcendentals=0),
        **kw,
    )


def vmem():
    return pl.BlockSpec(memory_space=pltpu.VMEM)


def swap(values, bits, count):
    return lax.ppermute(values, "ep", [(i, i ^ bits) for i in range(count)])


def join_kernel(*refs):
    for k, ref in enumerate(refs[:-1]):
        refs[-1][k] = ref[...]


def join(blocks, shape):
    return call(
        join_kernel,
        jax.ShapeDtypeStruct((len(blocks),) + shape, blocks[0].dtype),
        4,
        blocks[0].size,
        blocks[0].size,
        in_specs=[vmem()] * len(blocks),
        out_specs=vmem(),
        name="join",
    )(*blocks)


def gather(block, count, ahead, local_copy=None):
    blocks = [block if local_copy is None else local_copy]
    for k in reversed(range(1, count // 4)):
        blocks.append(swap(block, 4 * k, count))
    side = []
    for k in range(ahead):
        side.append(swap(blocks[k], 2, count))
    rest = early = join(blocks[ahead:], block.shape)
    rest = swap(rest, 2, count)
    if ahead:
        early = join(blocks + side, block.shape)
    early_core = swap(early, 1, count)
    return early, rest, early_core, swap(rest, 1, count)


def owners(me, parts, count, ahead):
    near = [0] + [4 * k for k in reversed(range(1, count // 4))]
    early = near + [bits ^ 2 for bits in near[:ahead]]
    rest = [bits ^ 2 for bits in near[ahead:]]
    every = early, rest, [bits ^ 1 for bits in early], [bits ^ 1 for bits in rest]
    for bits, part in zip(every, parts):
        for k in range(part.shape[0]):
            yield part, k, me ^ bits[k]


AHEAD = {"first": 0, "second": 2}


def widen_rows(ref, rows):
    groups, _, lanes = ref.shape
    per_group = HEADS // groups
    lines = [
        jnp.broadcast_to(ref[g, t : t + 1, :], (per_group, lanes))
        for t in range(rows)
        for g in range(groups)
    ]
    return jnp.concatenate(lines, axis=0).reshape(rows, HEADS, lanes)


def three_parts(values):
    high = values.astype(BF16)
    rest = values - high.astype(F32)
    mid = rest.astype(BF16)
    low = (rest - mid.astype(F32)).astype(BF16)
    return high, mid, low


def one_row(ref):
    values = ref[...].astype(F32)
    return jnp.concatenate([values[k : k + 1] for k in range(values.shape[0])], axis=1)


def to_column(row, rows):
    size = row.shape[1]
    i = lax.broadcasted_iota(jnp.int32, (rows, size), 0)
    j = lax.broadcasted_iota(jnp.int32, (rows, size), 1)
    return jnp.sum(jnp.where(i == j, jnp.broadcast_to(row, (rows, size)), 0.0), axis=1, keepdims=True)


def local_kernel(
    hidden_ref, gain_ref, b_ref, c_ref, dt_ref, conv_ref, taps_ref, bias_ref, dt_bias_ref,
    log_ref, skip_ref, ids_ref, prob_ref, score_ref,
    early_ref, coef_ref, step_ref, b_wide_ref, c_wide_ref, decay_ref, bc_ref, ids_out_ref, share_ref,
    own_ref, spread_ref,
):
    rows, _ = hidden_ref.shape
    inner = HEADS * HEAD_DIM
    span = SSM_GROUPS * STATE
    per_group = HEADS // SSM_GROUPS
    own_ref[...] = hidden_ref[...]
    values = hidden_ref[...].astype(F32)
    scale = lax.rsqrt(jnp.mean(values * values, axis=-1, keepdims=True) + EPS)
    normed = (values * scale * one_row(gain_ref)).astype(BF16)
    taps = taps_ref[...].astype(F32)
    last = taps.shape[0] - 1
    early = one_row(bias_ref)
    for k in range(last):
        early = early + conv_ref[k].astype(F32) * taps[k : k + 1]
    early_ref[...] = jnp.zeros_like(early_ref)
    early_ref[:rows] = early[:, :inner]
    width = share_ref.shape[1]
    split = share_ref.shape[0] // (3 * PAD)
    at = lax.broadcasted_iota(jnp.int32, (rows, width), 1)
    expert = (at // PAD).astype(F32)
    ids = [to_column(ids_ref[k : k + 1].astype(F32), rows) for k in range(TOP)]
    scores = score_ref[...]
    shares = prob_ref[...] * scores / jnp.sum(scores, axis=0, keepdims=True)
    shares = [to_column(shares[k : k + 1], rows) for k in range(TOP)]
    weight = jnp.zeros((rows, width), F32)
    used = jnp.zeros((rows, width), F32)
    numbers = jnp.zeros((rows, LANES), F32)
    lane = lax.broadcasted_iota(jnp.int32, (rows, LANES), 1)
    line = lax.broadcasted_iota(jnp.int32, (rows, LANES), 0)
    for k in range(TOP):
        hit = jnp.broadcast_to(ids[k], (rows, width)) == expert
        weight += jnp.where(hit, jnp.broadcast_to(shares[k], (rows, width)), 0.0)
        used += jnp.where(hit, 1.0, 0.0)
        numbers += jnp.where(lane == k * PAD + line, jnp.broadcast_to(ids[k] + 1.0, (rows, LANES)), 0.0)
    ids_out_ref[...] = jnp.sum(numbers, axis=0, keepdims=True) - 1.0
    seen = jnp.zeros((1, width), F32)
    ranks = []
    for t in range(rows):
        ranks.append(seen)
        seen = seen + used[t : t + 1]
    rank = jnp.concatenate(ranks, axis=0)
    weight = jnp.where(rank == (at % PAD // split).astype(F32), weight, 0.0)
    share_ref[...] = jnp.zeros_like(share_ref)
    for s in range(split):
        cut = jnp.where(at % split == s, weight, 0.0)
        for i, part in enumerate(three_parts(cut)):
            share_ref[(3 * s + i) * PAD : (3 * s + i) * PAD + rows] = part
    chan = lax.broadcasted_iota(jnp.int32, (HEADS, inner), 0)
    lane = lax.broadcasted_iota(jnp.int32, (HEADS, inner), 1)
    spread_ref[...] = (lane // HEAD_DIM == chan).astype(F32).astype(BF16)
    b_part = jnp.dot(normed, b_ref[...], preferred_element_type=F32).astype(BF16)
    c_part = jnp.dot(normed, c_ref[...], preferred_element_type=F32).astype(BF16)
    dt_raw = lax.dot_general(
        normed, dt_ref[...], (((1,), (1,)), ((), ())), preferred_element_type=F32
    ).astype(BF16)
    bc_ref[:, :span] = b_part
    bc_ref[:, span:] = c_part
    fresh = jnp.concatenate([b_part, c_part], axis=1).astype(F32)
    active = silu(early[:, inner:] + fresh * taps[last:, inner:])
    b_act = active[:, :span]
    c_act = active[:, span:]
    step = jax.nn.softplus(dt_raw.astype(F32) + dt_bias_ref[...])
    decay = jnp.exp(-step * jnp.exp(log_ref[...]))
    coefs = []
    for g in range(SSM_GROUPS):
        cut = slice(g * STATE, (g + 1) * STATE)
        b_wide_ref[g] = jnp.concatenate([b_act[:, cut]] * (LANES // STATE), axis=1)
        c_wide_ref[g] = jnp.concatenate([c_act[:, cut]] * (LANES // STATE), axis=1)
        dots = jnp.sum(b_act[:, cut] * c_act[:, cut], axis=1, keepdims=True)
        coefs.append(jnp.broadcast_to(dots, (rows, per_group)))
    coef = step * jnp.concatenate(coefs, axis=1) + skip_ref[...]
    blank = jnp.zeros((PAD - rows, HEADS), F32)
    parts = []
    for values in (coef, step):
        parts += three_parts(jnp.concatenate([values, blank], axis=0))
    wide = jnp.dot(jnp.concatenate(parts, axis=0), spread_ref[...], preferred_element_type=F32)
    for i, ref in enumerate((coef_ref, step_ref)):
        at = 3 * PAD * i
        ref[...] = wide[at : at + PAD] + wide[at + PAD : at + 2 * PAD] + wide[at + 2 * PAD : at + 3 * PAD]
    for t in range(rows):
        decay_ref[t] = jnp.broadcast_to(to_column(decay[t : t + 1], HEADS), (HEADS, LANES))


def read_kernel(
    state_ref, c_ref, decay_ref, out_ref, keep_ref, c_wide_ref, sums_ref, flat_ref, sems
):
    rows, heads, width = state_ref.shape
    lanes = 1024

    def copy(chunk):
        cut = pl.ds(pl.multiple_of(chunk * lanes, lanes), lanes)
        return pltpu.make_async_copy(
            state_ref.at[:, :, cut], keep_ref.at[:, :, cut], sems.at[chunk]
        )

    def begin(chunk, carry):
        copy(chunk).start()
        return carry

    lax.fori_loop(0, width // lanes, begin, 0)
    c_wide_ref[...] = widen_rows(c_ref, rows)
    sums_ref[...] = jnp.zeros_like(sums_ref)

    def one(chunk, carry):
        copy(chunk).wait()
        at = pl.multiple_of(chunk * lanes, lanes)
        prods = []
        for k in range(lanes // LANES):
            prod = keep_ref[:, :, pl.ds(at + k * LANES, LANES)] * c_wide_ref[...]
            prods.append(prod.reshape(rows * heads, LANES).astype(BF16))
        lane = lax.broadcasted_iota(jnp.int32, (lanes, HEAD_DIM), 0)
        chan = lax.broadcasted_iota(jnp.int32, (lanes, HEAD_DIM), 1)
        pick = (chunk * (lanes // STATE) + lane // STATE == chan).astype(F32).astype(BF16)
        prods = jnp.concatenate(prods, axis=1)
        sums_ref[...] += jnp.dot(prods, pick, preferred_element_type=F32)
        return carry

    lax.fori_loop(0, width // lanes, one, 0)
    flat_ref[...] = sums_ref[...] * decay_ref[...].reshape(rows * heads, LANES)[:, :HEAD_DIM]
    out_ref[...] = jnp.zeros_like(out_ref)
    for h in range(0, heads, 2):
        pair = [flat_ref[pl.ds(h + j, rows, stride=heads), :] for j in range(2)]
        out_ref[:rows, h * HEAD_DIM : (h + 2) * HEAD_DIM] = jnp.concatenate(pair, axis=1)


def read_state(state_in, c_wide, decay_wide):
    rows, heads, width = state_in.shape
    return call(
        read_kernel,
        jax.ShapeDtypeStruct((PAD, heads * HEAD_DIM), F32),
        20,
        20_000_000,
        state_in.size * 4,
        in_specs=[pl.BlockSpec(memory_space=pltpu.HBM), vmem(), vmem()],
        out_specs=vmem(),
        scratch_shapes=[
            pltpu.VMEM(state_in.shape, F32),
            pltpu.VMEM((rows, heads, LANES), F32),
            pltpu.VMEM((rows * heads, HEAD_DIM), F32),
            pltpu.VMEM((rows * heads, HEAD_DIM), F32),
            pltpu.SemaphoreType.DMA((width // 1024,)),
        ],
        name="read_state",
    )(state_in, c_wide, decay_wide)


def write_kernel(
    state_ref, xs_ref, b_ref, decay_ref, conv_ref, fresh_ref, bc_ref,
    out_ref, conv_out_ref, parts_ref, b_wide_ref, new_ref, in_sems, sems,
):
    rows, heads, width = state_ref.shape
    lanes = 512
    inner = heads * HEAD_DIM

    def fetch(chunk):
        cut = pl.ds(pl.multiple_of(chunk * lanes, lanes), lanes)
        return pltpu.make_async_copy(
            state_ref.at[:, :, cut], new_ref.at[:, :, cut], in_sems.at[chunk]
        )

    def begin(chunk, carry):
        fetch(chunk).start()
        return carry

    lax.fori_loop(0, width // lanes, begin, 0)
    for h in range(heads):
        parts_ref[pl.ds(h, rows, stride=heads), :] = xs_ref[
            :rows, h * HEAD_DIM : (h + 1) * HEAD_DIM
        ]
    parts = jnp.concatenate(three_parts(parts_ref[...]), axis=1)
    b_wide_ref[...] = widen_rows(b_ref, rows)

    def copy(chunk):
        cut = pl.ds(pl.multiple_of(chunk * lanes, lanes), lanes)
        return pltpu.make_async_copy(
            new_ref.at[:, :, cut], out_ref.at[:, :, cut], sems.at[chunk]
        )

    def one(chunk, carry):
        at = pl.multiple_of(chunk * lanes, lanes)
        lane = lax.broadcasted_iota(jnp.int32, (3 * HEAD_DIM, lanes), 1)
        chan = lax.broadcasted_iota(jnp.int32, (3 * HEAD_DIM, lanes), 0)
        spread = chunk * (lanes // STATE) + lane // STATE == chan % HEAD_DIM
        wide = jnp.dot(parts, spread.astype(F32).astype(BF16), preferred_element_type=F32)
        wide = wide.reshape(rows, heads, lanes)
        fetch(chunk).wait()
        for k in range(lanes // LANES):
            cut = pl.ds(at + k * LANES, LANES)
            new_ref[:, :, cut] = (
                decay_ref[...] * new_ref[:, :, cut]
                + wide[:, :, k * LANES : (k + 1) * LANES] * b_wide_ref[...]
            )
        copy(chunk).start()
        return carry

    lax.fori_loop(0, width // lanes, one, 0)
    taps = conv_ref.shape[0]
    for k in range(1, taps):
        conv_out_ref[k - 1] = conv_ref[k]
    conv_out_ref[taps - 1, :, :inner] = fresh_ref[:rows]
    conv_out_ref[taps - 1, :, inner:] = bc_ref[...]

    def done(chunk, carry):
        copy(chunk).wait()
        return carry

    lax.fori_loop(0, width // lanes, done, 0)


def write_state(state, xs, b_wide, decay_wide, conv, fresh, bc):
    rows, heads, width = state.shape
    return call(
        write_kernel,
        (jax.ShapeDtypeStruct(state.shape, F32), jax.ShapeDtypeStruct(conv.shape, BF16)),
        16,
        40_000_000,
        state.size * 8,
        in_specs=[pl.BlockSpec(memory_space=pltpu.HBM)] + [vmem()] * 6,
        out_specs=(pl.BlockSpec(memory_space=pltpu.HBM), vmem()),
        scratch_shapes=[
            pltpu.VMEM((rows * heads, HEAD_DIM), F32),
            pltpu.VMEM((rows, heads, LANES), F32),
            pltpu.VMEM(state.shape, F32),
            pltpu.SemaphoreType.DMA((width // 512,)),
            pltpu.SemaphoreType.DMA((width // 512,)),
        ],
        name="write_state",
    )(state, xs, b_wide, decay_wide, conv, fresh, bc)


def project_kernel(*refs):
    *parts, z_ref, x_ref, gain_ref, ids_ref, out_ref, rows_ref = refs
    me = lax.axis_index("ep")
    count = rows_ref.shape[0]
    rows, model_width = parts[0].shape[1:]
    cols = z_ref.shape[1]
    rows_ref[:, rows:, :] = jnp.zeros((count, PAD - rows, model_width), BF16)
    for part, k, owner in owners(me, parts, count, AHEAD["first"]):
        rows_ref[owner, :rows] = part[k]
    values = rows_ref[...].astype(F32).reshape(count * PAD, model_width)
    scale = lax.rsqrt(jnp.mean(values * values, axis=-1, keepdims=True) + EPS)
    normed = (values * scale * one_row(gain_ref)).astype(BF16)
    z_cols = jnp.dot(normed, z_ref[...], preferred_element_type=F32)
    x_cols = jnp.dot(normed, x_ref[...], preferred_element_type=F32).astype(BF16)
    spare = lax.broadcasted_iota(jnp.int32, (count * PAD, LANES), 0) % PAD == rows
    ids = jnp.broadcast_to(ids_ref[...], (count * PAD, LANES))
    first = jnp.where(spare, ids, z_cols[:, :LANES])
    z_cols = jnp.concatenate([first, z_cols[:, LANES:]], axis=1) if cols > LANES else first
    out_ref[:, :, :cols] = z_cols.astype(BF16).reshape(count, PAD, cols)
    out_ref[:, :, cols:] = x_cols.reshape(count, PAD, cols)


def gate_kernel(
    zx_ref, early_ref, taps_ref, coef_ref, read_ref, step_ref, gain_ref, y_ref, xs_ref, fresh_ref
):
    count, _, both = zx_ref.shape
    cols = both // 2
    inner = count * cols
    z = jnp.concatenate([zx_ref[j, :, :cols] for j in range(count)], axis=1)
    x = jnp.concatenate([zx_ref[j, :, cols:] for j in range(count)], axis=1)
    fresh_ref[...] = x
    last = taps_ref.shape[0] - 1
    tap = taps_ref[...].astype(F32)[last:, :inner]
    x_act = silu(early_ref[...] + x.astype(F32) * tap)
    xs_ref[...] = step_ref[...] * x_act
    gated = (read_ref[...] + coef_ref[...] * x_act) * silu(z.astype(F32))
    scale = lax.rsqrt(jnp.mean(gated * gated, axis=-1, keepdims=True) + EPS)
    y_ref[...] = (gated * scale * one_row(gain_ref)).astype(BF16)


def output_kernel(*refs):
    *parts, weight_ref, pick_ref, out_ref, cols_ref = refs
    count, slots, col = out_ref.shape
    width = weight_ref.shape[0]
    rows = jnp.concatenate(
        [part[...].reshape(part.shape[0] * PAD, width) for part in parts], axis=0
    )
    cols = jnp.dot(rows, weight_ref[...], preferred_element_type=F32)
    blocks = owners(lax.axis_index("ep"), parts, count, AHEAD["second"])
    for i, (_, _, owner) in enumerate(blocks):
        cols_ref[owner] = cols[i * PAD : (i + 1) * PAD]
    cols = cols_ref[...].reshape(count * PAD, col).astype(BF16)
    pick = pick_ref[...].reshape(count * slots, count * PAD)
    picked = jnp.dot(pick, cols, preferred_element_type=F32)
    out_ref[...] = picked.astype(BF16).reshape(count, slots, col)


def choose_kernel(zx_ref, rows_ref, pick_ref, hidden_ref, capacity, rows):
    count, slots, tokens = pick_ref.shape
    ids = jnp.concatenate(
        [zx_ref[j, :, :LANES].astype(F32)[rows : rows + 1] for j in range(count)], axis=0
    ).astype(BF16)
    source = lax.broadcasted_iota(jnp.int32, (LANES, tokens), 0)
    lane = lax.broadcasted_iota(jnp.int32, (LANES, tokens), 1)
    mine = lax.broadcasted_iota(jnp.int32, (count, tokens), 0)
    token = lax.broadcasted_iota(jnp.int32, (count, tokens), 1)
    named = jnp.zeros((count, tokens), F32)
    for k in range(TOP):
        take = (source == k * PAD + lane % PAD).astype(F32).astype(BF16)
        wide = jnp.dot(ids, take, preferred_element_type=F32)
        line = jnp.sum(jnp.where(mine == token // PAD, wide, 0.0), axis=0, keepdims=True)
        named += (jnp.broadcast_to(line, (count, tokens)) == mine.astype(F32)).astype(F32)
    row = lax.broadcasted_iota(jnp.int32, (tokens, tokens), 0)
    col = lax.broadcasted_iota(jnp.int32, (tokens, tokens), 1)
    before = ((row // PAD == col // PAD) & (row < col)).astype(F32).astype(BF16)
    place = jnp.dot(named.astype(BF16), before, preferred_element_type=F32)
    place = jnp.where(named > 0.5, place, -1.0)
    slot = lax.broadcasted_iota(jnp.int32, (slots, tokens), 0)
    lane = lax.broadcasted_iota(jnp.int32, (slots, tokens), 1)
    taken = slots - PAD
    from_sender = (slot // capacity == lane // PAD) & (slot < taken)
    wanted = jnp.where(from_sender, (slot % capacity).astype(F32), -2.0)
    for j in range(count):
        hit = wanted == jnp.broadcast_to(place[j : j + 1], (slots, tokens))
        own = lane - j * PAD == slot - taken
        pick_ref[j] = ((hit | (own & (slot >= taken)))).astype(F32).astype(BF16)
    mine = pick_ref[lax.axis_index("ep")]
    hidden = rows_ref[...].reshape(tokens, rows_ref.shape[2])
    hidden_ref[...] = jnp.dot(mine, hidden, preferred_element_type=F32).astype(BF16)


def expert_kernel(
    hidden_ref, cols_ref, gain_ref, gate_ref, up_ref, down_ref, out_ref, mixed_ref, capacity
):
    count, slots, _ = cols_ref.shape
    model_width = hidden_ref.shape[1]
    projected = jnp.concatenate([cols_ref[j] for j in range(count)], axis=1)
    mixed = (hidden_ref[...].astype(F32) + projected.astype(F32)).astype(BF16)
    mixed_ref[...] = mixed[slots - PAD :]
    wide = mixed.astype(F32)
    scale = lax.rsqrt(jnp.mean(wide * wide, axis=-1, keepdims=True) + EPS)
    normed = (wide * scale * one_row(gain_ref)).astype(BF16)
    gate = jnp.dot(normed, gate_ref[0], preferred_element_type=F32)
    up = jnp.dot(normed, up_ref[0], preferred_element_type=F32)
    act = (silu(gate) * up).astype(BF16)
    width = out_ref.shape[2]
    split = model_width // width
    tokens = count * PAD
    row = lax.broadcasted_iota(jnp.int32, (tokens, slots), 0)
    slot = lax.broadcasted_iota(jnp.int32, (tokens, slots), 1)
    place = row % PAD // split
    spread = (slot == row // PAD * capacity + place) & (place < capacity)
    act = jnp.dot(spread.astype(F32).astype(BF16), act, preferred_element_type=F32).astype(BF16)
    result = jnp.dot(act, down_ref[0], preferred_element_type=F32)
    row = lax.broadcasted_iota(jnp.int32, (tokens, width), 0) % split
    folded = result[:, :width]
    for s in range(1, split):
        folded = jnp.where(row == s, result[:, s * width : (s + 1) * width], folded)
    out_ref[...] = folded.astype(BF16).reshape(count, PAD, width)


def combine_kernel(back_ref, share_ref, mixed_ref, out_ref):
    count, _, width = back_ref.shape
    rows, model_width = out_ref.shape
    values = back_ref[...].reshape(count * PAD, width)
    sums = jnp.dot(share_ref[...], values, preferred_element_type=F32)
    for s in range(model_width // width):
        at = 3 * PAD * s
        total = sums[at : at + PAD] + sums[at + PAD : at + 2 * PAD] + sums[at + 2 * PAD : at + 3 * PAD]
        cut = slice(s * width, (s + 1) * width)
        out_ref[:, cut] = (mixed_ref[:, cut].astype(F32) + total)[:rows].astype(BF16)


def body(
    hidden,
    state_in,
    conv_state,
    expert_ids,
    group_prob,
    expert_score,
    first_gain,
    z_weight,
    x_weight,
    b_weight,
    c_weight,
    dt_weight,
    conv_weight,
    conv_bias,
    dt_bias,
    decay_log,
    skip_gain,
    inner_gain,
    out_weight,
    second_gain,
    expert_gate,
    expert_up,
    expert_down,
):
    rows, model_width = hidden.shape
    inner = HEADS * HEAD_DIM
    span = SSM_GROUPS * STATE
    count = lax.axis_size("ep")
    tokens = count * PAD
    capacity = max(2, (3 * rows * TOP + 2 * count - 1) // (2 * count))
    slots = 2
    while slots < capacity:
        slots *= 2
    split = PAD // slots

    def streamed(array):
        return pltpu.with_memory_space_constraint(array, pltpu.HBM)

    conv_state = conv_state.transpose(1, 0, 2)

    def lines(vector):
        return vector.reshape(-1, LANES)


    def wide(kind):
        return jax.ShapeDtypeStruct((PAD, inner), kind)

    early, coef, step, b_wide, c_wide, decay_wide, bc, ids_row, share_rows, own = call(
        local_kernel,
        (
            wide(F32),
            wide(F32),
            wide(F32),
            jax.ShapeDtypeStruct((SSM_GROUPS, rows, LANES), F32),
            jax.ShapeDtypeStruct((SSM_GROUPS, rows, LANES), F32),
            jax.ShapeDtypeStruct((rows, HEADS, LANES), F32),
            jax.ShapeDtypeStruct((rows, 2 * span), BF16),
            jax.ShapeDtypeStruct((1, LANES), F32),
            jax.ShapeDtypeStruct((split * 3 * PAD, tokens), BF16),
            jax.ShapeDtypeStruct(hidden.shape, BF16),
        ),
        16,
        10_000_000,
        4_000_000,
        in_specs=[vmem()] * 14,
        out_specs=(vmem(),) * 10,
        scratch_shapes=[pltpu.VMEM((HEADS, inner), BF16)],
        name="local",
    )(
        *[
            streamed(array)
            for array in (
                hidden,
                lines(first_gain),
                b_weight,
                c_weight,
                dt_weight.T,
                conv_state,
                conv_weight,
                lines(conv_bias),
                dt_bias[None, :],
                decay_log[None, :],
                skip_gain[None, :],
                expert_ids.T,
                group_prob[None, :],
                expert_score.T,
            )
        ]
    )
    parts = gather(hidden, count, AHEAD["first"], own)
    read = read_state(streamed(state_in), c_wide, decay_wide)

    cols = z_weight.shape[1]
    zx, all_rows = call(
        project_kernel,
        (
            jax.ShapeDtypeStruct((count, PAD, 2 * cols), BF16),
            jax.ShapeDtypeStruct((count, PAD, model_width), BF16),
        ),
        12,
        4 * tokens * model_width * cols,
        4 * model_width * cols,
        in_specs=[vmem()] * 8,
        out_specs=(vmem(), vmem()),
        name="project",
    )(*parts, z_weight, x_weight, lines(first_gain), ids_row)
    zx = lax.all_to_all(zx, "ep", split_axis=0, concat_axis=0, tiled=True)
    y_mix, xs, x_fresh = call(
        gate_kernel,
        (wide(BF16), wide(F32), wide(BF16)),
        8,
        40 * PAD * inner,
        30 * PAD * inner,
        in_specs=[vmem()] * 7,
        out_specs=(vmem(),) * 3,
        name="gate",
    )(zx, early, conv_weight, coef, read, step, lines(inner_gain))

    taken = count * capacity + PAD
    pick, chosen = call(
        functools.partial(choose_kernel, capacity=capacity, rows=rows),
        (
            jax.ShapeDtypeStruct((count, taken, tokens), BF16),
            jax.ShapeDtypeStruct((taken, model_width), BF16),
        ),
        8,
        2 * taken * tokens * model_width,
        2 * tokens * model_width,
        in_specs=[vmem()] * 2,
        out_specs=(vmem(), vmem()),
        name="choose",
    )(zx, all_rows)

    parts = gather(y_mix, count, AHEAD["second"])
    state_out, conv_out = write_state(
        streamed(state_in), xs, b_wide, decay_wide, conv_state, x_fresh, bc
    )
    out_cols = out_weight.shape[1]
    slab = call(
        output_kernel,
        jax.ShapeDtypeStruct((count, taken, out_cols), BF16),
        12,
        2 * tokens * inner * out_cols,
        2 * inner * out_cols,
        in_specs=[vmem()] * 6,
        out_specs=vmem(),
        scratch_shapes=[pltpu.VMEM((count, PAD, out_cols), F32)],
        name="output",
    )(*parts, out_weight, pick)

    slab = lax.all_to_all(slab, "ep", split_axis=0, concat_axis=0, tiled=True)
    back, mixed = call(
        functools.partial(expert_kernel, capacity=capacity),
        (
            jax.ShapeDtypeStruct((count, PAD, model_width // split), BF16),
            jax.ShapeDtypeStruct((PAD, model_width), BF16),
        ),
        24,
        6 * tokens * expert_gate.shape[1] * expert_gate.shape[2],
        6 * expert_gate.shape[1] * expert_gate.shape[2],
        in_specs=[vmem()] * 6,
        out_specs=(vmem(), vmem()),
        name="expert",
    )(chosen, slab, lines(second_gain), expert_gate, expert_up, expert_down)

    back = lax.all_to_all(back, "ep", split_axis=0, concat_axis=0, tiled=True)
    layer_out = call(
        combine_kernel,
        jax.ShapeDtypeStruct((rows, model_width), BF16),
        8,
        2 * 6 * PAD * tokens * model_width,
        2 * tokens * model_width,
        in_specs=[vmem()] * 3,
        out_specs=vmem(),
        name="combine",
    )(back, share_rows, mixed)
    return layer_out, state_out, conv_out.transpose(1, 0, 2)


def solution(mesh):
    seq = ("grp", "ep")
    in_specs = (
        P(seq, None),
        P(seq, None, None),
        P(seq, None, None),
        P(seq, None),
        P(seq),
        P(seq, None),
        P(),
        P(None, "ep"),
        P(None, "ep"),
        P(),
        P(),
        P(),
        P(),
        P(),
        P(),
        P(),
        P(),
        P(),
        P(None, "ep"),
        P(),
        P("ep", None, None),
        P("ep", None, None),
        P("ep", None, None),
    )
    out_specs = (P(seq, None), P(seq, None, None), P(seq, None, None))

    return jax.shard_map(body, mesh=mesh, in_specs=in_specs, out_specs=out_specs, check_vma=False)
```
